32 devices in a mesh: fs: 16 (over z, y, x), tp: 2 (over core).
Axes of the slice: x: 2, y: 2, z: 4, core: 2. Of those that a mesh axis runs over, the one named last changes fastest.
Arguments:
- saved_input: bfloat16 [16384, 2048], P('fs'), may hold values from -60 to 60
- out_cotangent: bfloat16 [16384, 4096], P('fs', 'tp'), may hold values from -6 to 6
- old_weight: float32 [2048, 4096], P('fs', 'tp'), may hold values from -0.125 to 0.125
- factor: bfloat16 [4096, 256], P('tp'), may hold values from -0.09375 to 0.09375
- moment_first: float32 [2048, 256], P('fs'), may hold values from -3 to 3
- moment_second: float32 [2048, 256], P('fs'), may hold values from 0.05 to 1
Outputs:
- new_weight: float32 [2048, 4096], P('fs', 'tp')
- update: float32 [2048, 4096], P('fs', 'tp')
- new_first: float32 [2048, 256], P('fs')
- new_second: float32 [2048, 256], P('fs')
- weight_copy: bfloat16 [2048, 4096], P(None, 'tp')
The draws below stay inside these ranges and needn't reach their ends.
All inputs are finite; a program needn't handle non-finite values.
Results may differ from the reference program's by a relative error of at most 0.0028.
Values may be sent and summed in bfloat16 or wider, within the bound.
A program may use at most 64 MiB of HBM per device.

```python
import math
import jax
import jax.numpy as jnp
from jax import lax

D = 4096
HV = 2048
RANK = 256
TOKENS = 16384


def draw_saved_input(key, part):
    first = jax.random.fold_in(jax.random.fold_in(key, 11), 0)
    column = jnp.arange(HV, dtype=jnp.float32) / HV
    scale = jnp.exp(column * 2.302585)
    values = jnp.clip(jax.random.normal(first, (TOKENS, HV), jnp.float32), -6.0, 6.0) * scale
    return values.astype(jnp.bfloat16)


def level_of(stream_key, extent, shards, least, largest):
    gain, own = 1.0, jax.random.fold_in(stream_key, 6)
    for position, parts in shards:
        draws = jnp.exp(jax.random.uniform(jax.random.fold_in(own, position), (parts,), jnp.float32, least / len(shards), largest / len(shards)))
        gain = gain * jnp.repeat(draws, extent[position] // parts).reshape([-1 if axis == position else 1 for axis in range(len(extent))])
    return gain


def noise(own_key, shape, width, limit, cuts=(), kind=jnp.bfloat16):
    values = jax.random.normal(own_key, shape, jnp.float32) * width
    if len(cuts) > 0:
        values = level_of(own_key, shape, cuts, -0.22, 0.18) * values
    return jnp.clip(values, min=-limit, max=limit).astype(kind)


def setup_inputs(seed: int = 0) -> dict:
    seeds = jax.random.split(jax.random.key(seed), 7)
    saved_input = draw_saved_input(jax.random.fold_in(seeds[6], 71), 0)
    out_cotangent = noise(seeds[1], (TOKENS, D), 1.0, 6.0, ((0, 16), (1, 2)))
    old_weight = noise(seeds[2], (HV, D), HV ** -0.5, 0.125, ((0, 16), (1, 2)), jnp.float32)
    factor = noise(seeds[3], (D, RANK), D ** -0.5, 0.09375, ((0, 2),))
    moment_first = noise(seeds[4], (HV, RANK), 0.5, 3.0, ((0, 16),), jnp.float32)
    moment_second = jnp.clip(jnp.exp(math.log(1.0) - 2.9957323 * jax.random.uniform(seeds[5], (HV, RANK), jnp.float32) ** level_of(seeds[5], (HV, RANK), ((0, 16),), -0.2, 0.2)), 0.05, 1.0)
    return {"saved_input": saved_input, "out_cotangent": out_cotangent, "old_weight": old_weight, "factor": factor, "moment_first": moment_first, "moment_second": moment_second}


def reference(saved_input, out_cotangent, old_weight, factor, moment_first, moment_second):
    gradient = jnp.dot(saved_input.T, out_cotangent, preferred_element_type=jnp.float32)
    wide_factor = factor.astype(jnp.float32)
    projected = jnp.dot(gradient, wide_factor, precision=lax.Precision.HIGHEST)
    total = jnp.sqrt(jnp.sum(projected * projected))
    clip = jnp.minimum(1.0, math.sqrt(HV * RANK) / (total + 1e-06))
    clipped = clip * projected
    new_first = 0.9 * moment_first + 0.1 * clipped
    new_second = 0.95 * moment_second + 0.05 * clipped * clipped
    direction = new_first / (jnp.sqrt(new_second) + 1e-08)
    update = jnp.dot(direction, wide_factor.T, precision=lax.Precision.HIGHEST)
    new_weight = old_weight - 0.05 * update
    return (new_weight, update, new_first, new_second, new_weight.astype(jnp.bfloat16))
```

```python
import functools
import math

import jax
import jax.numpy as jnp
from jax import lax
from jax.experimental import pallas as pl
from jax.experimental.pallas import tpu as pltpu
from jax.sharding import PartitionSpec as P

F32, BF16 = jnp.float32, jnp.bfloat16
MESH = pl.DeviceIdType.MESH
LIMIT = 0.125
SPAN = 120.0
SLOPE = 2 * SPAN / LIMIT


def encode(weight):
    size = jnp.exp2(jnp.abs(weight) * SLOPE - SPAN)
    return jnp.where(weight < 0, -size, size).astype(BF16)


def decode(code):
    code = code.astype(F32)
    size = jnp.log2(jnp.abs(code)) * (1 / SLOPE) + SPAN / SLOPE
    return jnp.where(code < 0, -size, size)


def plain(saved_input, out_cotangent, old_weight, factor, moment_first, moment_second):
    wide_factor = factor.astype(F32)
    contract = (((0,), (0,)), ((), ()))
    reduced = jnp.dot(out_cotangent, factor, preferred_element_type=F32)
    high = reduced.astype(BF16)
    low = (reduced - high.astype(F32)).astype(BF16)
    high_part = lax.dot_general(saved_input, high, contract, preferred_element_type=F32)
    low_part = lax.dot_general(saved_input, low, contract, preferred_element_type=F32)
    shard = lax.psum_scatter(high_part + low_part, ("fs", "tp"), scatter_dimension=0, tiled=True)
    projected = lax.all_gather(shard, "tp", axis=0, tiled=True)
    squares = lax.psum(jnp.sum(projected * projected), "fs")
    entries = saved_input.shape[1] * factor.shape[1]
    clip = jnp.minimum(1.0, math.sqrt(entries) / (jnp.sqrt(squares) + 1e-06))
    clipped = clip * projected
    new_first = 0.9 * moment_first + 0.1 * clipped
    new_second = 0.95 * moment_second + 0.05 * clipped * clipped
    direction = new_first / (jnp.sqrt(new_second) + 1e-08)
    update = jnp.dot(direction, wide_factor.T, precision=lax.Precision.HIGHEST)
    new_weight = old_weight - 0.05 * update
    copied = lax.all_gather(new_weight.astype(BF16), "fs", axis=0, tiled=True)
    return (new_weight, update, new_first, new_second, copied)


def exchange(n, entries, old, saved_hbm, cot_hbm, fac_hbm, m1, m2,
             gath, dirbuf, dirf, nf, ns,
             old16, saved, cot, fac, ybuf, pbuf, xbuf, sbuf, rbuf, projv, sqbuf,
             in_sem, own_sem, send_sem, recv_sem, pair_sem,
             ps_sem, pr_sem, qs_sem, qr_sem, ds_sem, dr_sem):
    me, c = lax.axis_index("fs"), lax.axis_index("tp")
    nz = n // 4
    x, y, z = lax.rem(me, 2), lax.rem(me // 2, 2), me // 4
    xn = me + 1 - 2 * x
    yn = me + 2 - 4 * y
    xyn = xn + 2 - 4 * y
    has_up, has_dn = z + 1 < nz, z > 0
    unit = old.shape[0] // 8
    parts = [(0, 3 * unit), (3 * unit, 3 * unit), (6 * unit, unit), (7 * unit, unit)]
    half = old.shape[0] // 2
    contract = (((0,), (0,)), ((), ()))

    loads = [pltpu.make_async_copy(a, b, in_sem.at[i])
             for i, (a, b) in enumerate([(cot_hbm, cot), (fac_hbm, fac), (saved_hbm, saved)])]
    for load in loads:
        load.start()
    barrier = pltpu.get_barrier_semaphore()

    def greet(k, _):
        pl.semaphore_signal(barrier, inc=1, device_id=(lax.rem(me + k, n), c), device_id_type=MESH)
        return 0

    lax.fori_loop(1, n, greet, 0)
    pl.semaphore_signal(barrier, inc=1, device_id=(me, 1 - c), device_id_type=MESH)
    piece = old.shape[0] // 4
    for k in range(4):
        old16[pl.ds(k * piece, piece)] = encode(old[pl.ds(k * piece, piece)])
    own_copy = pltpu.make_async_copy(old16, gath.at[me], own_sem)
    own_copy.start()
    pl.semaphore_wait(barrier, n)

    pending = []

    def send(cls, origin, target, own=False, cond=None):
        site = len(pending)
        first, count = parts[cls]

        def make():
            src = old16.at[pl.ds(first, count)] if own else gath.at[origin, pl.ds(first, count)]
            return pltpu.make_async_remote_copy(
                src, gath.at[origin, pl.ds(first, count)], send_sem.at[site],
                recv_sem.at[cls, origin], device_id=(target, c), device_id_type=MESH)

        pending.append((make, cond))
        if cond is None:
            make().start()
        else:
            @pl.when(cond)
            def _():
                make().start()

    def recv(cls, origin, cond=None):
        first, count = parts[cls]

        def wait():
            piece = gath.at[origin, pl.ds(first, count)]
            pltpu.make_async_remote_copy(
                piece, piece, send_sem.at[0], recv_sem.at[cls, origin],
                device_id=(me, c), device_id_type=MESH).wait_recv()

        if cond is None:
            wait()
        else:
            pl.when(cond)(wait)

    up, dn = me + 4, me - 4

    for cls, order in ((2, (xn, yn)), (3, (yn, xn))):
        for target in order:
            send(cls, me, target, own=True)
    for cls, order in ((0, (xn, yn)), (1, (yn, xn))):
        send(cls, me, up, own=True, cond=has_up)
        send(cls, me, dn, own=True, cond=has_dn)
        for target in order:
            send(cls, me, target, own=True)
    for cls in (2, 3):
        send(cls, me, up, own=True, cond=has_up)
        send(cls, me, dn, own=True, cond=has_dn)

    def sides(s):
        yield -4 * s, z >= s, up, has_up
        yield 4 * s, z + s < nz, dn, has_dn

    def a_line(cls, s):
        near = (xn, yn) if cls == 0 else (yn, xn)
        for shift, there, ahead, more in sides(s):
            recv(cls, me + shift, there)
            if s + 1 < nz:
                send(cls, me + shift, ahead, cond=jnp.logical_and(there, more))
            for target in near:
                send(cls, me + shift, target, cond=there)

    def a_cross(cls, s):
        near, far = (xn, yn) if cls == 0 else (yn, xn)
        if s == 0:
            recv(cls, near)
            send(cls, near, far)
            return
        for shift, there, _, _ in sides(s):
            recv(cls, near + shift, there)
            send(cls, near + shift, far, cond=there)

    def a_last(cls, s):
        near, far = (xn, yn) if cls == 0 else (yn, xn)
        for origin in (far, xyn):
            if s == 0:
                recv(cls, origin)
                continue
            for shift, there, _, _ in sides(s):
                recv(cls, origin + shift, there)

    def c_flat(cls, origin, forward=None):
        recv(cls, origin)
        if forward is not None:
            send(cls, origin, forward)
        send(cls, origin, up, cond=has_up)
        send(cls, origin, dn, cond=has_dn)

    def c_line(cls, s):
        for origin in (me, xn, yn, xyn) if cls == 2 else (me, yn, xn, xyn):
            for shift, there, ahead, more in sides(s):
                recv(cls, origin + shift, there)
                if s + 1 < nz:
                    send(cls, origin + shift, ahead, cond=jnp.logical_and(there, more))

    loads[0].wait()
    loads[1].wait()
    tall = cot.shape[0] // 4

    def reduce_rows(k, _):
        rows = pl.ds(pl.multiple_of(k * tall, tall), tall)
        value = jnp.dot(cot[rows, :], fac[...], preferred_element_type=F32)
        high = value.astype(BF16)
        ybuf[0, rows, :] = high
        ybuf[1, rows, :] = (value - high.astype(F32)).astype(BF16)
        return 0

    lax.fori_loop(0, 4, reduce_rows, 0)
    loads[2].wait()
    wide = 4 * half

    def project(k, _):
        cols = saved[:, pl.ds(pl.multiple_of(k * wide, wide), wide)]
        value = lax.dot_general(cols, ybuf[0], contract, preferred_element_type=F32)
        value = value + lax.dot_general(cols, ybuf[1], contract, preferred_element_type=F32)
        pbuf[pl.ds(2 * k, 2)] = value.reshape((2, 2, half, value.shape[1]))
        return 0

    lax.fori_loop(0, n // 2, project, 0)

    def pair_copy(i, src, dst):
        return pltpu.make_async_remote_copy(
            src, dst, pair_sem.at[2 * i], pair_sem.at[2 * i + 1],
            device_id=(me, 1 - c), device_id_type=MESH)

    swap = pair_copy(0, pbuf.at[:, 1 - c], xbuf)
    swap.start()

    a_line(0, 1)
    a_line(1, 1)
    c_flat(2, xn, yn)
    c_flat(3, yn, xn)

    swap.wait()

    def chip_sum(k, _):
        value = pbuf[k, c] + xbuf[k]
        xbuf[k] = value
        sbuf[k] = value.astype(BF16)
        return 0

    lax.fori_loop(0, n, chip_sum, 0)

    def to_owner(k):
        peer = lax.rem(me + k, n)
        return pltpu.make_async_remote_copy(
            sbuf.at[peer], rbuf.at[me], ps_sem.at[peer], pr_sem.at[me],
            device_id=(peer, c), device_id_type=MESH)

    def from_peer(k, buf, sem):
        peer = lax.rem(me + k, n)
        return pltpu.make_async_remote_copy(
            buf, buf, sem, sem, device_id=(me, c), device_id_type=MESH)

    def start_owner(k, _):
        to_owner(k).start()
        return 0

    lax.fori_loop(1, n, start_owner, 0)

    a_cross(0, 0)
    a_cross(1, 0)
    c_flat(2, yn)
    c_flat(3, xn)
    c_flat(2, xyn)
    c_flat(3, xyn)
    if nz > 2:
        a_line(0, 2)
        a_line(1, 2)
    a_cross(0, 1)
    a_cross(1, 1)

    def take(k, _):
        peer = lax.rem(me + k, n)
        from_peer(k, rbuf.at[peer], pr_sem.at[peer]).wait_recv()
        return 0

    lax.fori_loop(1, n, take, 0)

    def add(k, total):
        return total + rbuf[lax.rem(me + k, n)].astype(F32)

    projv[c] = lax.fori_loop(1, n, add, xbuf[me])
    share = pair_copy(1, projv.at[c], projv.at[c])
    share.start()
    c_line(2, 1)
    c_line(3, 1)
    share.wait()
    projected = projv[...]
    sqbuf[me] = jnp.full(sqbuf.shape[1:], jnp.sum(projected * projected), F32)

    def to_all(k):
        peer = lax.rem(me + k, n)
        return pltpu.make_async_remote_copy(
            sqbuf.at[me], sqbuf.at[me], qs_sem.at[peer], qr_sem.at[me],
            device_id=(peer, c), device_id_type=MESH)

    def start_all(k, _):
        to_all(k).start()
        return 0

    lax.fori_loop(1, n, start_all, 0)
    for s in range(3, nz):
        a_line(0, s)
        a_line(1, s)
    if nz > 2:
        a_cross(0, 2)
        a_cross(1, 2)
        c_line(2, 2)
        c_line(3, 2)

    def take_squares(k, _):
        peer = lax.rem(me + k, n)
        from_peer(k, sqbuf.at[peer], qr_sem.at[peer]).wait_recv()
        return 0

    lax.fori_loop(1, n, take_squares, 0)
    squares = sqbuf[0]
    for k in range(1, n):
        squares = squares + sqbuf[k]
    clip = jnp.minimum(1.0, math.sqrt(entries) / (jnp.sqrt(squares) + 1e-06))[0:1]
    for h in range(2):
        rows = pl.ds(h * half, half)
        clipped = clip * projv[h]
        first = 0.9 * m1[rows] + 0.1 * clipped
        second = 0.95 * m2[rows] + 0.05 * clipped * clipped
        nf[rows] = first
        ns[rows] = second
        dirf[rows] = first / (jnp.sqrt(second) + 1e-08)
    dirbuf[me, c] = dirf[pl.ds(pl.multiple_of(c * half, half), half)].astype(BF16)

    def direction_to(k):
        peer = lax.rem(me + k, n)
        return pltpu.make_async_remote_copy(
            dirbuf.at[me, c], dirbuf.at[me, c], ds_sem.at[peer], dr_sem.at[me],
            device_id=(peer, c), device_id_type=MESH)

    def start_direction(k, _):
        direction_to(k).start()
        return 0

    lax.fori_loop(1, n, start_direction, 0)
    for s in range(3, nz):
        a_cross(0, s)
        a_cross(1, s)
        c_line(2, s)
        c_line(3, s)

    def take_direction(k, _):
        peer = lax.rem(me + k, n)
        from_peer(k, dirbuf.at[peer, c], dr_sem.at[peer]).wait_recv()
        return 0

    lax.fori_loop(1, n, take_direction, 0)
    halves = pair_copy(2, dirbuf.at[:, c], dirbuf.at[:, c])
    halves.start()
    for s in range(nz):
        a_last(0, s)
        a_last(1, s)
    halves.wait()
    own_copy.wait()

    def finish(k, _):
        to_owner(k).wait_send()
        to_all(k).wait_send()
        direction_to(k).wait_send()
        return 0

    lax.fori_loop(1, n, finish, 0)
    for make, cond in pending:
        if cond is None:
            make().wait_send()
        else:
            @pl.when(cond)
            def _(make=make):
                make().wait_send()


def sites(nz):
    flat = 16 + 2 * 7
    line = sum((2 * 2 * 3 if s + 1 < nz else 2 * 2 * 2) for s in range(1, nz))
    cross = 2 * (1 + 2 * (nz - 1))
    columns = sum(2 * 4 * 2 for s in range(1, nz) if s + 1 < nz)
    return flat + line + cross + columns


def overlapped(n, saved_input, out_cotangent, old_weight, factor, moment_first, moment_second):
    rows, width = old_weight.shape
    rank = factor.shape[1]
    half = rows // 2
    entries = saved_input.shape[1] * rank
    any_space = pl.BlockSpec(memory_space=pl.ANY)
    vmem = pl.BlockSpec(memory_space=pltpu.VMEM)
    shape = jax.ShapeDtypeStruct
    sem = pltpu.SemaphoreType.DMA
    gath, dirbuf, direction, new_first, new_second = pl.pallas_call(
        functools.partial(exchange, n, entries),
        out_shape=[
            shape((n, rows, width), BF16),
            shape((n, 2, half, rank), BF16),
            shape((rows, rank), F32),
            shape((rows, rank), F32),
            shape((rows, rank), F32),
        ],
        in_specs=[vmem, any_space, any_space, any_space, vmem, vmem],
        out_specs=[any_space, vmem, vmem, vmem, vmem],
        scratch_shapes=[
            pltpu.VMEM((rows, width), BF16),
            pltpu.VMEM(saved_input.shape, BF16),
            pltpu.VMEM(out_cotangent.shape, BF16),
            pltpu.VMEM(factor.shape, BF16),
            pltpu.VMEM((2, saved_input.shape[0], rank), BF16),
            pltpu.VMEM((n, 2, half, rank), F32),
            pltpu.VMEM((n, half, rank), F32),
            pltpu.VMEM((n, half, rank), BF16),
            pltpu.VMEM((n, half, rank), BF16),
            pltpu.VMEM((2, half, rank), F32),
            pltpu.VMEM((n, 8, rank), F32),
            sem((3,)), sem, sem((sites(n // 4),)), sem((4, n)), sem((6,)),
            sem((n,)), sem((n,)), sem((n,)), sem((n,)), sem((n,)), sem((n,)),
        ],
        compiler_params=pltpu.CompilerParams(
            collective_id=0, has_side_effects=True, vmem_limit_bytes=48 * 2**20
        ),
    )(old_weight, saved_input, out_cotangent, factor, moment_first, moment_second)
    across = (((1,), (1,)), ((), ()))
    every = lax.dot_general(
        dirbuf.reshape((n * rows, rank)), factor, across, preferred_element_type=F32
    )
    copied = (decode(gath.reshape((n * rows, width))) - 0.05 * every).astype(BF16)
    update = lax.dot_general(
        direction, factor.astype(F32), across, precision=lax.Precision.HIGHEST
    )
    new_weight = old_weight - 0.05 * update
    return (new_weight, update, new_first, new_second, copied)


def solution(mesh):
    n, pair = mesh.shape["fs"], mesh.shape["tp"]

    def on_device(*args):
        rows = args[2].shape[0]
        if pair == 2 and n % 4 == 0 and n >= 8 and rows % 128 == 0:
            return overlapped(n, *args)
        return plain(*args)

    return jax.shard_map(
        on_device,
        mesh=mesh,
        in_specs=(
            P("fs", None),
            P("fs", "tp"),
            P("fs", "tp"),
            P("tp", None),
            P("fs", None),
            P("fs", None),
        ),
        out_specs=(P("fs", "tp"), P("fs", "tp"), P("fs", None), P("fs", None), P(None, "tp")),
        check_vma=False,
    )
```
